128 devices in a mesh: fs: 16 (over z, x), tp: 8 (over y, core).
Axes of the slice: x: 4, y: 4, z: 4, core: 2. Of those that a mesh axis runs over, the one named last changes fastest.
Arguments:
- h_saved: bfloat16 [32768, 2048], P('fs'), may hold values from -6 to 6
- conv_cotan: bfloat16 [32768, 2560], P('fs', 'tp'), may hold values from -64 to 64
- lru_out: bfloat16 [32768, 2560], P('fs', 'tp'), may hold values from -64 to 64
- out_cotan: bfloat16 [32768, 2048], P('fs'), may hold values from -6 to 6
- basis_in: bfloat16 [2048, 256], P('fs'), may hold values from -1.41421356 to 1.41421356
- basis_out: bfloat16 [2048, 256], P('fs'), may hold values from -1.41421356 to 1.41421356
- weight_in: float32 [2048, 2560], P('fs', 'tp'), may hold values from -0.125 to 0.125
- weight_out: float32 [2560, 2048], P('tp', 'fs'), may hold values from -0.125 to 0.125
- first_in: float32 [256, 2560], P('fs', 'tp'), may hold values from -6 to 6
- second_in: float32 [256, 2560], P('fs', 'tp'), may hold values from 0.05 to 2
- first_out: float32 [256, 2560], P('fs', 'tp'), may hold values from -6 to 6
- second_out: float32 [256, 2560], P('fs', 'tp'), may hold values from 0.05 to 2
Outputs:
- step_in: float32 [2048, 2560], P('fs', 'tp')
- new_weight_in: float32 [2048, 2560], P('fs', 'tp')
- copy_in: bfloat16 [2048, 2560], P(None, 'tp')
- new_first_in: float32 [256, 2560], P('fs', 'tp')
- new_second_in: float32 [256, 2560], P('fs', 'tp')
- step_out: float32 [2560, 2048], P('tp', 'fs')
- new_weight_out: float32 [2560, 2048], P('tp', 'fs')
- copy_out: bfloat16 [2560, 2048], P('tp')
- new_first_out: float32 [256, 2560], P('fs', 'tp')
- new_second_out: float32 [256, 2560], P('fs', 'tp')
The draws below stay inside these ranges and needn't reach their ends.
All inputs are finite; a program needn't handle non-finite values.
Results may differ from the reference program's by a relative error of at most 0.0046.
Values may be sent and summed in bfloat16 or wider, within the bound.
No kernel may reach another device: no remote copies, remote signals or barrier semaphores. Data moves between devices by JAX's collectives and lax.ppermute only.
A program may use at most 128 MiB of HBM per device.

```python
import math
import jax
import jax.numpy as jnp
from jax import lax

D_MODEL = 2048
D_RNN = 2560
RANK = 256
TOKENS = 32768


def scaled_field(key, count, columns):
    keyone, keytwo = jax.random.split(key, 2)
    place = jnp.arange(columns, dtype=jnp.float32) / max(columns - 1, 1)
    rough = jnp.exp(jax.random.uniform(keytwo, (columns,), jnp.float32, math.log(0.5), math.log(2.0)))
    column_scale = jnp.exp(math.log(3.0) * place) * rough
    values = jnp.clip(jax.random.normal(keyone, (count, columns), jnp.float32), -6.0, 6.0)
    return values * column_scale


def draw_conv_cotan(key, part):
    return scaled_field(jax.random.fold_in(key, 11), TOKENS, D_RNN).astype(jnp.bfloat16)


def draw_lru_out(key, part):
    return scaled_field(jax.random.fold_in(key, 12), TOKENS, D_RNN).astype(jnp.bfloat16)


def draw_basis_in(key, part):
    return (scaled_field(jax.random.fold_in(key, 13), D_MODEL, RANK) / math.sqrt(D_MODEL)).astype(jnp.bfloat16)


def draw_basis_out(key, part):
    return (scaled_field(jax.random.fold_in(key, 14), D_MODEL, RANK) / math.sqrt(D_MODEL)).astype(jnp.bfloat16)


def block_scale(rng, dims, pieces, smallest, largest):
    level = 1.0
    for axis_at, blocks in pieces:
        steps = jax.random.uniform(jax.random.fold_in(jax.random.fold_in(rng, 6), axis_at), (blocks,), jnp.float32, smallest / len(pieces), largest / len(pieces))
        level = level * jnp.repeat(jnp.exp(steps), dims[axis_at] // blocks).reshape((-1,) + (1,) * (len(dims) - 1 - axis_at))
    return level


def scatter_about(stream_key, dims, width, most, shards=(), kind=jnp.bfloat16):
    loudness = block_scale(stream_key, dims, shards, -0.22, 0.18) if shards else 1.0
    values = jax.random.normal(stream_key, dims, jnp.float32) * width * loudness
    return jnp.minimum(jnp.maximum(values, -most), most).astype(kind)


def setup_inputs(seed: int = 0) -> dict:
    key_list = jax.random.split(jax.random.key(seed), 13)
    return {
        "h_saved": scatter_about(key_list[0], (TOKENS, D_MODEL), 1.0, 6.0, ((0, 16),)),
        "conv_cotan": draw_conv_cotan(jax.random.fold_in(key_list[12], 71), 0),
        "lru_out": draw_lru_out(jax.random.fold_in(key_list[12], 71), 0),
        "out_cotan": scatter_about(key_list[3], (TOKENS, D_MODEL), 1.0, 6.0, ((0, 16),)),
        "basis_in": draw_basis_in(jax.random.fold_in(key_list[12], 71), 0),
        "basis_out": draw_basis_out(jax.random.fold_in(key_list[12], 71), 0),
        "weight_in": scatter_about(key_list[6], (D_MODEL, D_RNN), D_MODEL ** -0.5, 0.125, ((0, 16), (1, 8)), jnp.float32),
        "weight_out": scatter_about(key_list[7], (D_RNN, D_MODEL), D_RNN ** -0.5, 0.125, ((0, 8), (1, 16)), jnp.float32),
        "first_in": scatter_about(key_list[8], (RANK, D_RNN), 1.0, 6.0, ((0, 16), (1, 8)), jnp.float32),
        "second_in": jnp.clip(jnp.exp(math.log(2.0) - 3.6888794 * jax.random.uniform(key_list[9], (RANK, D_RNN), jnp.float32) ** block_scale(key_list[9], (RANK, D_RNN), ((0, 16), (1, 8)), -0.2, 0.2)), 0.05, 2.0),
        "first_out": scatter_about(key_list[10], (RANK, D_RNN), 1.0, 6.0, ((0, 16), (1, 8)), jnp.float32),
        "second_out": jnp.clip(jnp.exp(math.log(2.0) - 3.6888794 * jax.random.uniform(key_list[11], (RANK, D_RNN), jnp.float32) ** block_scale(key_list[11], (RANK, D_RNN), ((0, 16), (1, 8)), -0.2, 0.2)), 0.05, 2.0),
    }


def exact_dot(left, right):
    return jnp.dot(left.astype(jnp.float32), right.astype(jnp.float32), precision=lax.Precision.HIGHEST)

def projected(inputs, cotan, basis):
    grad = exact_dot(inputs.T, cotan)
    return jnp.dot(basis.astype(jnp.float32).T, grad, precision=lax.Precision.HIGHEST)

def moments(proj, factor, first, second):
    scaled = factor * proj
    first_new = 0.8 * first + 0.2 * scaled
    second_new = 0.9 * second + 0.1 * scaled * scaled
    direction = (first_new / (jnp.sqrt(second_new) + 1e-08)).astype(jnp.bfloat16)
    return (first_new, second_new, direction)

def reference(h_saved, conv_cotan, lru_out, out_cotan, basis_in, basis_out, weight_in, weight_out, first_in, second_in, first_out, second_out):
    proj_in = projected(h_saved, conv_cotan, basis_in)
    proj_out = projected(out_cotan, lru_out, basis_out)
    total = jnp.sum(proj_in * proj_in) + jnp.sum(proj_out * proj_out)
    factor = math.sqrt(2.0 * RANK * D_RNN) * lax.rsqrt(total + 1e-06)
    first_a, second_a, dir_in = moments(proj_in, factor, first_in, second_in)
    first_b, second_b, dir_out = moments(proj_out, factor, first_out, second_out)
    step_in = exact_dot(basis_in, dir_in)
    step_out = exact_dot(basis_out, dir_out).T
    new_in = weight_in - 0.02 * step_in
    new_out = weight_out - 0.02 * step_out
    return (step_in, new_in, new_in.astype(jnp.bfloat16), first_a, second_a, step_out, new_out, new_out.astype(jnp.bfloat16), first_b, second_b)
```

```python
import math

import jax
import jax.numpy as jnp
from jax import lax
from jax.sharding import Mesh
from jax.sharding import PartitionSpec as P

D_RNN = 2560
RANK = 256
FS = ("fs_0", "fs_1")
TP = ("tp_0", "tp_1")
EVERY = ("fs_0", "fs_1", "tp_0", "tp_1")
BF16 = jnp.bfloat16
F32 = jnp.float32


def sent_to_all(array, axis):
    copies = jnp.broadcast_to(array, (lax.axis_size(axis), *array.shape))
    return lax.all_to_all(copies, axis, split_axis=0, concat_axis=0, tiled=True)


def swapped(array):
    return lax.ppermute(array, "tp_1", [(0, 1), (1, 0)])


def moments(proj, factor, first, second):
    scaled = factor * proj
    first_new = 0.8 * first + 0.2 * scaled
    second_new = 0.9 * second + 0.1 * scaled * scaled
    direction = (first_new / (jnp.sqrt(second_new) + 1e-08)).astype(BF16)
    return (first_new, second_new, direction)


def contract(a, b, dims):
    return lax.dot_general(a, b, (dims, ((), ())), preferred_element_type=F32)


def shards(
    h_saved,
    conv_cotan,
    lru_out,
    out_cotan,
    basis_in,
    basis_out,
    weight_in,
    weight_out,
    first_in,
    second_in,
    first_out,
    second_out,
):
    takes_in = lax.axis_index("tp_1") == 0
    width = weight_in.shape[1]

    both = jnp.concatenate((weight_in.T, weight_out), axis=0).astype(BF16)
    mine, both = lax.optimization_barrier((jnp.where(takes_in, basis_in, basis_out), both))
    old = lax.all_gather(both, FS, axis=1, tiled=True)
    basis_own = sent_to_all(mine, FS).reshape(-1, RANK)
    tokens_own = jnp.where(takes_in, h_saved, out_cotan)
    wide_own = jnp.where(takes_in, conv_cotan.T, lru_out.T)
    wide_other = jnp.where(takes_in, lru_out.T, conv_cotan.T)
    tokens_own, wide_own, wide_other = lax.optimization_barrier((tokens_own, wide_own, wide_other))

    reduced_own = jnp.dot(tokens_own, basis_own, preferred_element_type=F32).astype(BF16)
    reduced_other = swapped(reduced_own)
    basis_other = swapped(basis_own)
    part_own = contract(reduced_own, wide_own, ((0,), (1,)))
    part_other = contract(reduced_other, wide_other, ((0,), (1,)))
    part = jnp.concatenate(
        (
            jnp.where(takes_in, part_own, part_other),
            jnp.where(takes_in, part_other, part_own),
        ),
        axis=1,
    ).astype(BF16)
    arrived = lax.all_to_all(
        part.reshape(16, RANK // 16, 2 * width), FS, split_axis=0, concat_axis=0, tiled=True
    )
    proj = arrived.astype(F32).sum(axis=0)
    partial_total = jnp.broadcast_to(jnp.sum(proj * proj), (1, 128))
    total = jnp.sum(sent_to_all(partial_total, EVERY)[:, 0, 0])
    factor = math.sqrt(2.0 * RANK * D_RNN) * lax.rsqrt(total + 1e-06)
    first_a, second_a, dir_in = moments(proj[:, :width], factor, first_in, second_in)
    first_b, second_b, dir_out = moments(proj[:, width:], factor, first_out, second_out)
    full = sent_to_all(jnp.concatenate((dir_in, dir_out), axis=1), FS).reshape(RANK, 2 * width)
    full_in, full_out = full[:, :width], full[:, width:]

    step_in = contract(basis_in, full_in, ((1,), (0,)))
    step_out = contract(full_out, basis_out, ((0,), (1,)))
    new_in = weight_in - 0.02 * step_in
    new_out = weight_out - 0.02 * step_out

    whole_in = jnp.where(takes_in, basis_own, basis_other)
    whole_out = jnp.where(takes_in, basis_other, basis_own)
    copy_in = old[:width].astype(F32) - 0.02 * contract(full_in, whole_in, ((0,), (1,)))
    copy_out = old[width:].astype(F32) - 0.02 * contract(full_out, whole_out, ((0,), (1,)))
    return (
        step_in,
        new_in,
        copy_in.astype(BF16).T,
        first_a,
        second_a,
        step_out,
        new_out,
        copy_out.astype(BF16),
        first_b,
        second_b,
    )


def solution(mesh):
    finer = Mesh(mesh.devices.reshape(4, 4, 4, 2), EVERY)
    placed = (
        P(FS, None),
        P(FS, TP),
        P(FS, TP),
        P(FS, None),
        P(FS, None),
        P(FS, None),
        P(FS, TP),
        P(TP, FS),
        P(FS, TP),
        P(FS, TP),
        P(FS, TP),
        P(FS, TP),
    )
    return jax.shard_map(
        shards,
        mesh=finer,
        in_specs=placed,
        out_specs=(
            P(FS, TP),
            P(FS, TP),
            P(None, TP),
            P(FS, TP),
            P(FS, TP),
            P(TP, FS),
            P(TP, FS),
            P(TP, None),
            P(FS, TP),
            P(FS, TP),
        ),
        check_vma=False,
    )
```

```python
import math

import jax
import jax.numpy as jnp
from jax import lax
from jax.experimental import pallas as pl
from jax.experimental.pallas import tpu as pltpu
from jax.sharding import Mesh
from jax.sharding import PartitionSpec as P

D_RNN = 2560
RANK = 256
FS = ("fs_0", "fs_1")
TP = ("tp_0", "tp_1")
EVERY = ("fs_0", "fs_1", "tp_0", "tp_1")
BF16 = jnp.bfloat16
F32 = jnp.float32

W = 320
ROWS = 16
PEERS = 16
SIDE = 4

LIMIT = pltpu.CompilerParams(vmem_limit_bytes=20 << 20)
VMEM = pl.BlockSpec(memory_space=pltpu.VMEM)
SMEM = pl.BlockSpec(memory_space=pltpu.SMEM)


def swapped(array):
    return lax.ppermute(array, "tp_1", [(0, 1), (1, 0)])


def shifted(array, axis, by):
    return lax.ppermute(array, axis, [(i, (i + by) % SIDE) for i in range(SIDE)])


def sent_to_all(array, axis):
    copies = jnp.broadcast_to(array, (lax.axis_size(axis), *array.shape))
    return lax.all_to_all(copies, axis, split_axis=0, concat_axis=0, tiled=True)


def contract(a, b, dims):
    return lax.dot_general(a, b, (dims, ((), ())), preferred_element_type=F32)


def pack_kernel(w_in, w_out, out):
    out[0:W, :] = w_in[...].astype(BF16)
    out[W : 2 * W, :] = w_out[...].astype(BF16)


def pack(*args):
    return pl.pallas_call(
        pack_kernel,
        out_shape=jax.ShapeDtypeStruct((2 * W, 128), BF16),
        in_specs=[VMEM] * 2,
        out_specs=VMEM,
        name="pack",
        compiler_params=LIMIT,
        cost_estimate=pl.CostEstimate(flops=10**6, bytes_accessed=500_000, transcendentals=0),
    )(*args)


def grads_kernel(where, conv, lru, h, o, keep, send):
    takes_in = where[0] == 0
    g_in = jnp.dot(conv[...], h[...], preferred_element_type=F32)
    g_out = jnp.dot(lru[...], o[...], preferred_element_type=F32)
    keep[...] = jnp.where(takes_in, g_in, g_out).astype(BF16)
    send[...] = jnp.where(takes_in, g_out, g_in).astype(BF16)


def grads(where, conv, lru, h, o):
    tile = 256
    wide = pl.BlockSpec((W, 2048), lambda i: (0, 0))
    tall = pl.BlockSpec((2048, tile), lambda i: (0, i))
    out = pl.BlockSpec((W, tile), lambda i: (0, i))
    return pl.pallas_call(
        grads_kernel,
        grid=(2048 // tile,),
        in_specs=[SMEM, wide, wide, tall, tall],
        out_specs=(out, out),
        out_shape=(jax.ShapeDtypeStruct((W, 2048), BF16),) * 2,
        name="grads",
        compiler_params=pltpu.CompilerParams(vmem_limit_bytes=57 << 20),
        cost_estimate=pl.CostEstimate(
            flops=4 * 2048 * 2048 * W, bytes_accessed=22_000_000, transcendentals=0
        ),
    )(where, conv, lru, h, o)


def project_kernel(kept, came, basis, out, total):
    n = pl.program_id(0)
    mine = jnp.dot(kept[...], basis[...], preferred_element_type=F32)
    other = jnp.dot(came[...], basis[...], preferred_element_type=F32)

    @pl.when(n == 0)
    def _():
        total[0:W] = mine
        total[W:] = other

    @pl.when(n > 0)
    def _():
        total[0:W] += mine
        total[W:] += other

    @pl.when(n == pl.num_programs(0) - 1)
    def _():
        out[...] = total[...].T.astype(BF16)


def project(kept, came, basis):
    tile = 512
    wide = pl.BlockSpec((W, tile), lambda i: (0, i))
    return pl.pallas_call(
        project_kernel,
        grid=(2048 // tile,),
        in_specs=[wide, wide, pl.BlockSpec((tile, RANK), lambda i: (i, 0))],
        out_specs=pl.BlockSpec((RANK, 2 * W), lambda i: (0, 0)),
        out_shape=jax.ShapeDtypeStruct((RANK, 2 * W), BF16),
        scratch_shapes=[pltpu.VMEM((2 * W, RANK), F32)],
        name="project",
        compiler_params=LIMIT,
        cost_estimate=pl.CostEstimate(
            flops=4 * 2048 * RANK * W, bytes_accessed=4_000_000, transcendentals=0
        ),
    )(kept, came, basis)


def moments(proj, factor, first, second):
    scaled = factor * proj
    first_new = 0.8 * first + 0.2 * scaled
    second_new = 0.9 * second + 0.1 * scaled * scaled
    direction = (first_new / (jnp.sqrt(second_new) + 1e-08)).astype(BF16)
    return (first_new, second_new, direction)


ORDER_Z = (0, 1, 3, 2)
ORDER_X = (0, 1, 3, 2)


def final_kernel(
    where,
    full,
    b_in,
    b_out,
    w_in,
    w_out,
    basis_own,
    basis_other,
    old_0,
    old_1,
    old_3,
    old_2a,
    old_2b,
    step_in,
    new_in,
    copy_in,
    step_out,
    new_out,
    copy_out,
    turned,
    s_in,
    s_out,
):
    takes_in = where[0] == 0
    n = pl.program_id(0)

    @pl.when(n == 0)
    def _():
        turned[...] = full[...].astype(F32).T.astype(BF16)
        own_in = contract(turned[0:W], b_in[...], ((1,), (1,)))
        own_out = contract(turned[W:], b_out[...], ((1,), (1,)))
        step_in[...] = own_in
        step_out[...] = own_out
        new_in[...] = w_in[...] - 0.02 * own_in
        new_out[...] = w_out[...] - 0.02 * own_out

    own = basis_own[...]
    other = basis_other[...]
    s_in[...] = contract(turned[0:W], jnp.where(takes_in, own, other), ((1,), (1,)))
    s_out[...] = contract(turned[W:], jnp.where(takes_in, other, own), ((1,), (1,)))

    def write(block, k):
        at = lax.rem(where[1] + ORDER_X[k], SIDE)
        cols = pl.ds(pl.multiple_of(at * 128, 128), 128)
        block = block.astype(F32)
        copy_in[:, cols] = (block[0:W] - 0.02 * s_in[:, cols]).astype(BF16)
        copy_out[:, cols] = (block[W:] - 0.02 * s_out[:, cols]).astype(BF16)

    for step, old in enumerate((old_0, old_1, old_3)):

        @pl.when(n == step)
        def _():
            for k in range(SIDE):
                write(old[k], k)

    @pl.when(n == 3)
    def _():
        for k in range(SIDE):
            write(old_2a[k] if k < 2 else old_2b[k - 2], k)


def final(where, full, bases, weights, own, other, old):
    shape = jax.ShapeDtypeStruct

    def whole(s):
        return pl.BlockSpec(s, lambda i, where: (0,) * len(s))

    tall = whole((W, 128))
    tile = pl.BlockSpec((512, RANK), lambda i, where: (where[2 + i], 0))
    copy = pl.BlockSpec((W, 512), lambda i, where: (0, where[2 + i]))
    return pl.pallas_call(
        final_kernel,
        grid_spec=pltpu.PrefetchScalarGridSpec(
            num_scalar_prefetch=1,
            grid=(SIDE,),
            in_specs=[
                whole((RANK, 2 * W)),
                whole((128, RANK)),
                whole((128, RANK)),
                tall,
                tall,
                tile,
                tile,
                *[whole((SIDE, 2 * W, 128))] * 3,
                *[whole((2, 2 * W, 128))] * 2,
            ],
            out_specs=(tall, tall, copy, tall, tall, copy),
            scratch_shapes=[
                pltpu.VMEM((2 * W, RANK), BF16),
                pltpu.VMEM((W, 512), F32),
                pltpu.VMEM((W, 512), F32),
            ],
        ),
        out_shape=(
            shape((W, 128), F32),
            shape((W, 128), F32),
            shape((W, 2048), BF16),
            shape((W, 128), F32),
            shape((W, 128), F32),
            shape((W, 2048), BF16),
        ),
        name="final",
        compiler_params=LIMIT,
        cost_estimate=pl.CostEstimate(
            flops=700_000_000, bytes_accessed=10_000_000, transcendentals=0
        ),
    )(where, full, *bases, *weights, own, other, *old)


def shards(
    h_saved,
    conv_cotan,
    lru_out,
    out_cotan,
    basis_in,
    basis_out,
    weight_in,
    weight_out,
    first_in,
    second_in,
    first_out,
    second_out,
):
    core = lax.axis_index("tp_1").astype(jnp.int32)
    at_z = lax.axis_index("fs_0").astype(jnp.int32)
    at_x = lax.axis_index("fs_1").astype(jnp.int32)
    takes_in = core == 0
    where = jnp.stack([core, at_x, *((at_z + d) & (SIDE - 1) for d in ORDER_Z)])

    mine = jnp.where(takes_in, basis_in, basis_out)
    basis_own = sent_to_all(mine, FS).reshape(-1, RANK)
    basis_other = swapped(basis_own)

    packed = pack(weight_in.T, weight_out)
    pieces = [packed]
    for d in ORDER_X[1:]:
        pieces.append(shifted(packed, "fs_1", -d))
    bundle = lax.optimization_barrier(jnp.stack(pieces))
    bundle_1 = shifted(bundle, "fs_0", -1)
    bundle_3 = shifted(bundle, "fs_0", -3)
    bundle_2a = shifted(bundle_1[:2], "fs_0", -1)
    bundle_2b = shifted(bundle_3[2:], "fs_0", -3)
    old = (bundle, bundle_1, bundle_3, bundle_2a, bundle_2b)

    kept, given = grads(where, conv_cotan.T, lru_out.T, h_saved, out_cotan)
    came = swapped(given)
    part = project(kept, came, basis_own)
    arrived = lax.all_to_all(
        part.reshape(PEERS, ROWS, 2 * W), FS, split_axis=0, concat_axis=0, tiled=True
    )
    proj = arrived.astype(F32).sum(axis=0)
    partial_total = jnp.broadcast_to(jnp.sum(proj * proj), (1, 128))
    total = jnp.sum(sent_to_all(partial_total, EVERY)[:, 0, 0])
    proj_own = proj[:, :W]
    proj_other = swapped(proj[:, W:])
    proj_in = jnp.where(takes_in, proj_own, proj_other)
    proj_out = jnp.where(takes_in, proj_other, proj_own)
    factor = math.sqrt(2.0 * RANK * D_RNN) * lax.rsqrt(total + 1e-06)
    first_a, second_a, dir_in = moments(proj_in, factor, first_in, second_in)
    first_b, second_b, dir_out = moments(proj_out, factor, first_out, second_out)
    full = sent_to_all(jnp.concatenate((dir_in, dir_out), axis=1), FS).reshape(RANK, 2 * W)
    step_in, new_in, copy_in, step_out, new_out, copy_out = final(
        where, full, (basis_in, basis_out), (weight_in.T, weight_out), basis_own, basis_other, old
    )
    return (
        step_in.T,
        new_in.T,
        copy_in.T,
        first_a,
        second_a,
        step_out,
        new_out,
        copy_out,
        first_b,
        second_b,
    )


def solution(mesh):
    finer = Mesh(mesh.devices.reshape(4, 4, 4, 2), EVERY)
    placed = (
        P(FS, None),
        P(FS, TP),
        P(FS, TP),
        P(FS, None),
        P(FS, None),
        P(FS, None),
        P(FS, TP),
        P(TP, FS),
        P(FS, TP),
        P(FS, TP),
        P(FS, TP),
        P(FS, TP),
    )
    return jax.shard_map(
        shards,
        mesh=finer,
        in_specs=placed,
        out_specs=(
            P(FS, TP),
            P(FS, TP),
            P(None, TP),
            P(FS, TP),
            P(FS, TP),
            P(TP, FS),
            P(TP, FS),
            P(TP, None),
            P(FS, TP),
            P(FS, TP),
        ),
        check_vma=False,
    )
```

```python
import functools
import math

import jax
import jax.numpy as jnp
from jax import lax
from jax.experimental import pallas as pl
from jax.experimental.pallas import tpu as pltpu
from jax.sharding import Mesh
from jax.sharding import PartitionSpec as P

D_RNN = 2560
RANK = 256
FS = ("fs_0", "fs_1")
TP = ("tp_0", "tp_1")
EVERY = ("fs_0", "fs_1", "tp_0", "tp_1")
BF16 = jnp.bfloat16
F32 = jnp.float32

W = 320
ROWS = 16
PEERS = 16
SIDE = 4

LIMIT = pltpu.CompilerParams(vmem_limit_bytes=20 << 20)
VMEM = pl.BlockSpec(memory_space=pltpu.VMEM)
SMEM = pl.BlockSpec(memory_space=pltpu.SMEM)


def swapped(array):
    return lax.ppermute(array, "tp_1", [(0, 1), (1, 0)])


def shifted(array, axis, by):
    return lax.ppermute(array, axis, [(i, (i + by) % SIDE) for i in range(SIDE)])


def contract(a, b, dims):
    return lax.dot_general(a, b, (dims, ((), ())), preferred_element_type=F32)


def pack_kernel(core, w_in, w_out, b_in, b_out, weights, bases):
    weights[0:W, :] = w_in[...].astype(BF16)
    weights[W : 2 * W, :] = w_out[...].astype(BF16)
    mine = jnp.where(core[0] == 0, b_in[...], b_out[...])
    for i in range(PEERS):
        bases[i] = mine


def pack(*args):
    return pl.pallas_call(
        pack_kernel,
        out_shape=(
            jax.ShapeDtypeStruct((2 * W, 128), BF16),
            jax.ShapeDtypeStruct((PEERS, 128, RANK), BF16),
        ),
        grid=(1,),
        in_specs=[
            SMEM,
            pl.BlockSpec((W, 128), lambda i: (0, 0)),
            pl.BlockSpec((W, 128), lambda i: (0, 0)),
            pl.BlockSpec((128, RANK), lambda i: (0, 0)),
            pl.BlockSpec((128, RANK), lambda i: (0, 0)),
        ],
        out_specs=(
            pl.BlockSpec((2 * W, 128), lambda i: (0, 0)),
            pl.BlockSpec((PEERS, 128, RANK), lambda i: (0, 0, 0)),
        ),
        name="pack",
        cost_estimate=pl.CostEstimate(flops=10**6, bytes_accessed=500_000, transcendentals=0),
    )(*args)


GRAD_TILE = 512
GRAD_TILES = 2048 // GRAD_TILE


def grad_kernel(flip, core, conv, lru, h, o, out, wide, tall, sems):
    uses_in = core[0] == flip

    def tile(source, k):
        cols = slice(k * GRAD_TILE, (k + 1) * GRAD_TILE)
        return pltpu.make_async_copy(source.at[:, cols], tall.at[k], sems.at[k])

    def factor(source):
        return pltpu.make_async_copy(source, wide, sems.at[GRAD_TILES])

    @pl.when(uses_in)
    def _():
        factor(conv).start()
        for k in range(GRAD_TILES):
            tile(h, k).start()

    @pl.when(jnp.logical_not(uses_in))
    def _():
        factor(lru).start()
        for k in range(GRAD_TILES):
            tile(o, k).start()

    factor(conv).wait()
    for k in range(GRAD_TILES):
        tile(h, k).wait()
        out[:, k * GRAD_TILE : (k + 1) * GRAD_TILE] = jnp.dot(
            wide[...], tall[k], preferred_element_type=F32
        ).astype(BF16)


def grad(flip, core, conv, lru, h, o):
    return pl.pallas_call(
        functools.partial(grad_kernel, flip),
        in_specs=[SMEM] + [pl.BlockSpec(memory_space=pltpu.HBM)] * 4,
        out_specs=VMEM,
        out_shape=jax.ShapeDtypeStruct((W, 2048), BF16),
        scratch_shapes=[
            pltpu.VMEM((W, 2048), BF16),
            pltpu.VMEM((GRAD_TILES, 2048, GRAD_TILE), BF16),
            pltpu.SemaphoreType.DMA((GRAD_TILES + 1,)),
        ],
        name="grad",
        compiler_params=pltpu.CompilerParams(vmem_limit_bytes=63 << 20),
        cost_estimate=pl.CostEstimate(
            flops=2 * 2048 * 2048 * W, bytes_accessed=11_000_000, transcendentals=0
        ),
    )(core, conv, lru, h, o)


PROJECT_TILES = 4


def project_kernel(kept, came, basis, out, kept_in, came_in, basis_in, sems):
    depth = 2048 // PROJECT_TILES
    copies = []
    for k in range(PROJECT_TILES):
        at = slice(k * depth, (k + 1) * depth)
        copies.append(
            (
                pltpu.make_async_copy(basis.at[at], basis_in.at[k], sems.at[0, k]),
                pltpu.make_async_copy(kept.at[:, at], kept_in.at[k], sems.at[1, k]),
                pltpu.make_async_copy(came.at[:, at], came_in.at[k], sems.at[2, k]),
            )
        )
    for group in copies:
        for copy in group:
            copy.start()
    mine = jnp.zeros((W, RANK), F32)
    other = jnp.zeros((W, RANK), F32)
    for k in range(PROJECT_TILES):
        for copy in copies[k]:
            copy.wait()
        mine = mine + jnp.dot(kept_in[k], basis_in[k], preferred_element_type=F32)
        other = other + jnp.dot(came_in[k], basis_in[k], preferred_element_type=F32)
    out[:, 0:W] = mine.T.astype(BF16)
    out[:, W:] = other.T.astype(BF16)


def project(kept, came, basis):
    depth = 2048 // PROJECT_TILES
    return pl.pallas_call(
        project_kernel,
        in_specs=[pl.BlockSpec(memory_space=pltpu.HBM)] * 3,
        out_specs=VMEM,
        out_shape=jax.ShapeDtypeStruct((RANK, 2 * W), BF16),
        scratch_shapes=[
            pltpu.VMEM((PROJECT_TILES, W, depth), BF16),
            pltpu.VMEM((PROJECT_TILES, W, depth), BF16),
            pltpu.VMEM((PROJECT_TILES, depth, RANK), BF16),
            pltpu.SemaphoreType.DMA((3, PROJECT_TILES)),
        ],
        name="project",
        compiler_params=pltpu.CompilerParams(vmem_limit_bytes=63 << 20),
        cost_estimate=pl.CostEstimate(
            flops=4 * 2048 * RANK * W, bytes_accessed=4_000_000, transcendentals=0
        ),
    )(kept, came, basis)


def collect_kernel(arrived, kept, given, squares):
    total = arrived[0].astype(F32)
    for i in range(1, PEERS):
        total = total + arrived[i].astype(F32)
    kept[...] = total[:, 0:W]
    given[...] = total[:, W:]
    sum_ = jnp.sum(jnp.sum(total * total, axis=0, keepdims=True), axis=1, keepdims=True)
    squares[...] = jnp.broadcast_to(sum_.reshape(1, 1, 1), (128, 1, 128))


def collect(arrived):
    return pl.pallas_call(
        collect_kernel,
        out_shape=(
            jax.ShapeDtypeStruct((ROWS, W), F32),
            jax.ShapeDtypeStruct((ROWS, W), F32),
            jax.ShapeDtypeStruct((128, 1, 128), F32),
        ),
        in_specs=[VMEM],
        out_specs=(VMEM,) * 3,
        name="collect",
        compiler_params=LIMIT,
        cost_estimate=pl.CostEstimate(flops=10**6, bytes_accessed=500_000, transcendentals=0),
    )(arrived)


def apply_kernel(
    core, totals, kept, came, old, nf_in, nv_in, nf_out, nv_out, dirs
):
    takes_in = core[0] == 0
    total = jnp.sum(totals[...], axis=0)[:, 0:1]
    factor = math.sqrt(2.0 * RANK * D_RNN) * lax.rsqrt(total + 1e-06)
    mine = kept[...]
    other = came[...]

    def moments(scaled, at, new_first, new_second):
        first = 0.8 * old[at : at + ROWS] + 0.2 * scaled
        second = 0.9 * old[at + ROWS : at + 2 * ROWS] + 0.1 * scaled * scaled
        new_first[...] = first
        new_second[...] = second
        return (first / (jnp.sqrt(second) + 1e-08)).astype(BF16)

    both = jnp.concatenate(
        (
            moments(factor * jnp.where(takes_in, mine, other), 0, nf_in, nv_in),
            moments(factor * jnp.where(takes_in, other, mine), 2 * ROWS, nf_out, nv_out),
        ),
        axis=1,
    )
    for i in range(PEERS):
        dirs[i] = both


def apply(*args):
    row = jax.ShapeDtypeStruct((ROWS, W), F32)
    return pl.pallas_call(
        apply_kernel,
        out_shape=(row, row, row, row, jax.ShapeDtypeStruct((PEERS, ROWS, 2 * W), BF16)),
        in_specs=[SMEM] + [VMEM] * 4,
        out_specs=(VMEM,) * 5,
        name="apply",
        compiler_params=LIMIT,
        cost_estimate=pl.CostEstimate(flops=10**6, bytes_accessed=500_000, transcendentals=0),
    )(*args)


def swap_last(n):
    return n ^ (n >> 1)


def final_kernel(
    core,
    at_x,
    at_z,
    full,
    bases,
    weights,
    basis_own,
    basis_other,
    old_0a,
    old_0b,
    old_1a,
    old_1b,
    old_3a,
    old_3b,
    old_2a,
    old_2b,
    step_in,
    new_in,
    copy_in,
    step_out,
    new_out,
    copy_out,
    turned,
):
    takes_in = core[0] == 0
    n = pl.program_id(0)

    @pl.when(n == 0)
    def _():
        turned[...] = full[...].astype(F32).T.astype(BF16)
        own_in = contract(turned[0:W], bases[0:128], ((1,), (1,)))
        own_out = contract(turned[W:], bases[128:], ((1,), (1,)))
        step_in[...] = own_in
        step_out[...] = own_out
        new_in[...] = weights[0:W] - 0.02 * own_in
        new_out[...] = weights[W:] - 0.02 * own_out

    own = basis_own[...]
    other = basis_other[...]

    def write(block_of):
        s_in = contract(turned[0:W], jnp.where(takes_in, own, other), ((1,), (1,)))
        s_out = contract(turned[W:], jnp.where(takes_in, other, own), ((1,), (1,)))
        for k in range(SIDE):
            block = block_of(swap_last((k - at_x[0]) & (SIDE - 1))).astype(F32)
            cols = slice(128 * k, 128 * (k + 1))
            copy_in[:, cols] = (block[0:W] - 0.02 * s_in[:, cols]).astype(BF16)
            copy_out[:, cols] = (block[W:] - 0.02 * s_out[:, cols]).astype(BF16)

    pairs = ((old_0a, old_0b), (old_1a, old_1b), (old_3a, old_3b), (old_2a, old_2b))
    for step, (near, far) in enumerate(pairs):

        @pl.when(n == step)
        def _():
            write(lambda r: jnp.where(r < 2, near[r & 1], far[r & 1]))


def final(core, at_x, at_z, full, bases, weights, own, other, old):
    shape = jax.ShapeDtypeStruct

    def whole(s):
        return pl.BlockSpec(s, lambda *_: (0,) * len(s))

    def place(i, at_z):
        return (at_z[0] + swap_last(i)) & (SIDE - 1)

    tall = whole((W, 128))
    tile = pl.BlockSpec((512, RANK), lambda i, core, at_x, at_z: (place(i, at_z), 0))
    copy = pl.BlockSpec((W, 512), lambda i, core, at_x, at_z: (0, place(i, at_z)))
    return pl.pallas_call(
        final_kernel,
        grid_spec=pltpu.PrefetchScalarGridSpec(
            num_scalar_prefetch=3,
            grid=(SIDE,),
            in_specs=[
                whole((RANK, 2 * W)),
                whole((2 * 128, RANK)),
                whole((2 * W, 128)),
                tile,
                tile,
                *[whole((2, 2 * W, 128))] * 8,
            ],
            out_specs=(tall, tall, copy, tall, tall, copy),
            scratch_shapes=[pltpu.VMEM((2 * W, RANK), BF16)],
        ),
        out_shape=(
            shape((W, 128), F32),
            shape((W, 128), F32),
            shape((W, 2048), BF16),
            shape((W, 128), F32),
            shape((W, 128), F32),
            shape((W, 2048), BF16),
        ),
        name="final",
        compiler_params=LIMIT,
        cost_estimate=pl.CostEstimate(
            flops=700_000_000, bytes_accessed=10_000_000, transcendentals=0
        ),
    )(core, at_x, at_z, full, bases, weights, own, other, *old)


def shards(
    h_saved,
    conv_cotan,
    lru_out,
    out_cotan,
    basis_in,
    basis_out,
    weight_in,
    weight_out,
    first_in,
    second_in,
    first_out,
    second_out,
):
    core = lax.axis_index("tp_1").astype(jnp.int32).reshape(1)
    at_z = lax.axis_index("fs_0").astype(jnp.int32).reshape(1)
    at_x = lax.axis_index("fs_1").astype(jnp.int32).reshape(1)

    packed, bases = pack(core, weight_in.T, weight_out, basis_in, basis_out)

    basis_own = lax.all_to_all(bases, FS, 0, 0, tiled=True).reshape(-1, RANK)
    basis_other = swapped(basis_own)

    pieces = [packed]
    for d in (1, 3, 2):
        pieces.append(shifted(packed, "fs_1", -d))
    halves = [lax.optimization_barrier(jnp.stack(pieces[k : k + 2])) for k in (0, 2)]
    old = list(halves)
    for d in (1, 3):
        for k in range(2):
            old.append(shifted(halves[k], "fs_0", -d))
    old.append(shifted(old[2], "fs_0", -1))
    old.append(shifted(old[5], "fs_0", -3))

    wide = (conv_cotan.T, lru_out.T, h_saved, out_cotan)
    given = grad(1, core, *wide)
    came = swapped(given)
    kept = grad(0, core, *wide)
    part = project(kept, came, basis_own)
    arrived = lax.all_to_all(
        part.reshape(PEERS, ROWS, 2 * W), FS, split_axis=0, concat_axis=0, tiled=True
    )
    old_moments = lax.optimization_barrier(
        jnp.concatenate((first_in, second_in, first_out, second_out), axis=0)
    )
    old_weights = lax.optimization_barrier(
        jnp.concatenate((weight_in.T, weight_out), axis=0)
    )
    own_bases = lax.optimization_barrier(jnp.concatenate((basis_in, basis_out), axis=0))
    proj_own, proj_given, squares = collect(arrived)
    totals = lax.all_to_all(squares, EVERY, 0, 0, tiled=True)
    proj_other = swapped(proj_given)
    first_a, second_a, first_b, second_b, dirs = apply(
        core, totals, proj_own, proj_other, old_moments
    )
    full = lax.all_to_all(dirs, FS, 0, 0, tiled=True).reshape(RANK, 2 * W)
    step_in, new_in, copy_in, step_out, new_out, copy_out = final(
        core, at_x, at_z, full, own_bases, old_weights, basis_own, basis_other, old
    )
    return (
        step_in.T,
        new_in.T,
        copy_in.T,
        first_a,
        second_a,
        step_out,
        new_out,
        copy_out,
        first_b,
        second_b,
    )


def solution(mesh):
    finer = Mesh(mesh.devices.reshape(4, 4, 4, 2), EVERY)
    placed = (
        P(FS, None),
        P(FS, TP),
        P(FS, TP),
        P(FS, None),
        P(FS, None),
        P(FS, None),
        P(FS, TP),
        P(TP, FS),
        P(FS, TP),
        P(FS, TP),
        P(FS, TP),
        P(FS, TP),
    )
    return jax.shard_map(
        shards,
        mesh=finer,
        in_specs=placed,
        out_specs=(
            P(FS, TP),
            P(FS, TP),
            P(None, TP),
            P(FS, TP),
            P(FS, TP),
            P(TP, FS),
            P(TP, FS),
            P(TP, None),
            P(FS, TP),
            P(FS, TP),
        ),
        check_vma=False,
    )
```

```python
import math

import jax
import jax.numpy as jnp
from jax import lax
from jax.experimental import pallas as pl
from jax.experimental.pallas import tpu as pltpu
from jax.sharding import Mesh
from jax.sharding import PartitionSpec as P

D_RNN = 2560
RANK = 256
FS = ("fs_0", "fs_1")
TP = ("tp_0", "tp_1")
EVERY = ("fs_0", "fs_1", "tp_0", "tp_1")
BF16 = jnp.bfloat16
F32 = jnp.float32

W = 320
ROWS = 16
PEERS = 16
SIDE = 4

LIMIT = pltpu.CompilerParams(vmem_limit_bytes=20 << 20)
VMEM = pl.BlockSpec(memory_space=pltpu.VMEM)
SMEM = pl.BlockSpec(memory_space=pltpu.SMEM)


def swapped(array):
    return lax.ppermute(array, "tp_1", [(0, 1), (1, 0)])


def shifted(array, axis, by):
    return lax.ppermute(array, axis, [(i, (i + by) % SIDE) for i in range(SIDE)])


def contract(a, b, dims):
    return lax.dot_general(a, b, (dims, ((), ())), preferred_element_type=F32)


def pack_kernel(core, at_x, at_z, w_in, w_out, b_in, b_out, weights, bases):
    weights[0:W, :] = w_in[...].astype(BF16)
    weights[W : 2 * W, :] = w_out[...].astype(BF16)
    mine = jnp.where(core[0] == 0, b_in[...], b_out[...])
    for i in range(PEERS):
        bases[i] = mine


def pack(*args):
    return pl.pallas_call(
        pack_kernel,
        out_shape=(
            jax.ShapeDtypeStruct((2 * W, 128), BF16),
            jax.ShapeDtypeStruct((PEERS, 128, RANK), BF16),
        ),
        grid=(1,),
        in_specs=[
            SMEM,
            SMEM,
            SMEM,
            pl.BlockSpec((W, 128), lambda i: (0, 0)),
            pl.BlockSpec((W, 128), lambda i: (0, 0)),
            pl.BlockSpec((128, RANK), lambda i: (0, 0)),
            pl.BlockSpec((128, RANK), lambda i: (0, 0)),
        ],
        out_specs=(
            pl.BlockSpec((2 * W, 128), lambda i: (0, 0)),
            pl.BlockSpec((PEERS, 128, RANK), lambda i: (0, 0, 0)),
        ),
        name="pack",
        cost_estimate=pl.CostEstimate(flops=10**6, bytes_accessed=500_000, transcendentals=0),
    )(*args)


GRAD_TILE = 512
GRAD_TILES = 2048 // GRAD_TILE


def grad_kernel(core, conv, conv_came, lru, lru_came, h, o, out, wide, tall, sems):
    def tile(source, k):
        cols = slice(k * GRAD_TILE, (k + 1) * GRAD_TILE)
        return pltpu.make_async_copy(source.at[:, cols], tall.at[k], sems.at[k])

    def half(source, k):
        return pltpu.make_async_copy(
            source, wide.at[k * W : (k + 1) * W], sems.at[GRAD_TILES + k]
        )

    def start(own, came, source):
        half(own, 0).start()
        half(came, 1).start()
        for k in range(GRAD_TILES):
            tile(source, k).start()

    @pl.when(core[0] == 0)
    def _():
        start(conv, conv_came, h)

    @pl.when(core[0] != 0)
    def _():
        start(lru, lru_came, o)

    half(conv, 0).wait()
    half(conv_came, 1).wait()
    for k in range(GRAD_TILES):
        tile(h, k).wait()
        out[:, k * GRAD_TILE : (k + 1) * GRAD_TILE] = jnp.dot(
            wide[...], tall[k], preferred_element_type=F32
        ).astype(BF16)


def grad(*args):
    return pl.pallas_call(
        grad_kernel,
        in_specs=[SMEM] + [pl.BlockSpec(memory_space=pltpu.HBM)] * 6,
        out_specs=VMEM,
        out_shape=jax.ShapeDtypeStruct((2 * W, 2048), BF16),
        scratch_shapes=[
            pltpu.VMEM((2 * W, 2048), BF16),
            pltpu.VMEM((GRAD_TILES, 2048, GRAD_TILE), BF16),
            pltpu.SemaphoreType.DMA((GRAD_TILES + 2,)),
        ],
        name="grad",
        compiler_params=pltpu.CompilerParams(vmem_limit_bytes=63 << 20),
        cost_estimate=pl.CostEstimate(
            flops=4 * 2048 * 2048 * W, bytes_accessed=14_000_000, transcendentals=0
        ),
    )(*args)


PROJECT_TILES = 4


def project_kernel(grads, basis, out, grads_in, basis_in, sems):
    depth = 2048 // PROJECT_TILES
    copies = []
    for k in range(PROJECT_TILES):
        at = slice(k * depth, (k + 1) * depth)
        copies.append(
            (
                pltpu.make_async_copy(basis.at[at], basis_in.at[k], sems.at[0, k]),
                pltpu.make_async_copy(grads.at[:, at], grads_in.at[k], sems.at[1, k]),
            )
        )
    for group in copies:
        for copy in group:
            copy.start()
    mine = jnp.zeros((W, RANK), F32)
    other = jnp.zeros((W, RANK), F32)
    for k in range(PROJECT_TILES):
        for copy in copies[k]:
            copy.wait()
        mine = mine + jnp.dot(grads_in[k, 0:W], basis_in[k], preferred_element_type=F32)
        other = other + jnp.dot(grads_in[k, W:], basis_in[k], preferred_element_type=F32)
    out[:, 0:W] = mine.T.astype(BF16)
    out[:, W:] = other.T.astype(BF16)


def project(grads, basis):
    depth = 2048 // PROJECT_TILES
    return pl.pallas_call(
        project_kernel,
        in_specs=[pl.BlockSpec(memory_space=pltpu.HBM)] * 2,
        out_specs=VMEM,
        out_shape=jax.ShapeDtypeStruct((RANK, 2 * W), BF16),
        scratch_shapes=[
            pltpu.VMEM((PROJECT_TILES, 2 * W, depth), BF16),
            pltpu.VMEM((PROJECT_TILES, depth, RANK), BF16),
            pltpu.SemaphoreType.DMA((2, PROJECT_TILES)),
        ],
        name="project",
        compiler_params=pltpu.CompilerParams(vmem_limit_bytes=63 << 20),
        cost_estimate=pl.CostEstimate(
            flops=4 * 2048 * RANK * W, bytes_accessed=4_000_000, transcendentals=0
        ),
    )(grads, basis)


def collect_kernel(arrived, kept, given, squares):
    total = arrived[0].astype(F32)
    for i in range(1, PEERS):
        total = total + arrived[i].astype(F32)
    kept[...] = total[:, 0:W]
    given[...] = total[:, W:]
    sum_ = jnp.sum(jnp.sum(total * total, axis=0, keepdims=True), axis=1, keepdims=True)
    squares[...] = jnp.broadcast_to(sum_.reshape(1, 1, 1), (128, 1, 128))


def collect(arrived):
    return pl.pallas_call(
        collect_kernel,
        out_shape=(
            jax.ShapeDtypeStruct((ROWS, W), F32),
            jax.ShapeDtypeStruct((ROWS, W), F32),
            jax.ShapeDtypeStruct((128, 1, 128), F32),
        ),
        in_specs=[VMEM],
        out_specs=(VMEM,) * 3,
        name="collect",
        compiler_params=LIMIT,
        cost_estimate=pl.CostEstimate(flops=10**6, bytes_accessed=500_000, transcendentals=0),
    )(arrived)


def apply_kernel(
    core, totals, kept, came, old, nf_in, nv_in, nf_out, nv_out, dirs
):
    takes_in = core[0] == 0
    total = jnp.sum(totals[...], axis=0)[:, 0:1]
    factor = math.sqrt(2.0 * RANK * D_RNN) * lax.rsqrt(total + 1e-06)
    mine = kept[...]
    other = came[...]

    def moments(scaled, at, new_first, new_second):
        first = 0.8 * old[at : at + ROWS] + 0.2 * scaled
        second = 0.9 * old[at + ROWS : at + 2 * ROWS] + 0.1 * scaled * scaled
        new_first[...] = first
        new_second[...] = second
        return (first / (jnp.sqrt(second) + 1e-08)).astype(BF16)

    both = jnp.concatenate(
        (
            moments(factor * jnp.where(takes_in, mine, other), 0, nf_in, nv_in),
            moments(factor * jnp.where(takes_in, other, mine), 2 * ROWS, nf_out, nv_out),
        ),
        axis=1,
    )
    for i in range(PEERS):
        dirs[i] = both


def apply(*args):
    row = jax.ShapeDtypeStruct((ROWS, W), F32)
    return pl.pallas_call(
        apply_kernel,
        out_shape=(row, row, row, row, jax.ShapeDtypeStruct((PEERS, ROWS, 2 * W), BF16)),
        in_specs=[SMEM] + [VMEM] * 4,
        out_specs=(VMEM,) * 5,
        name="apply",
        compiler_params=LIMIT,
        cost_estimate=pl.CostEstimate(flops=10**6, bytes_accessed=500_000, transcendentals=0),
    )(*args)


def swap_last(n):
    return n ^ (n >> 1)


def final_kernel(
    core,
    at_x,
    at_z,
    full,
    mark,
    bases,
    weights,
    basis_own,
    basis_other,
    old_0a,
    old_0b,
    old_1a,
    old_1b,
    old_3a,
    old_3b,
    old_2a,
    old_2b,
    step_in,
    new_in,
    copy_in,
    step_out,
    new_out,
    copy_out,
    turned,
):
    takes_in = core[0] == 0
    n = pl.program_id(0)

    @pl.when(n == 0)
    def _():
        turned[...] = full[...].astype(F32).T.astype(BF16)
        own_in = contract(turned[0:W], bases[0:128], ((1,), (1,)))
        own_out = contract(turned[W:], bases[128:], ((1,), (1,)))
        step_in[...] = own_in
        step_out[...] = own_out
        new_in[...] = weights[0:W] - 0.02 * own_in
        new_out[...] = weights[W:] - 0.02 * own_out

    own = basis_own[...]
    other = basis_other[...]

    def write(block_of):
        s_in = contract(turned[0:W], jnp.where(takes_in, own, other), ((1,), (1,)))
        s_out = contract(turned[W:], jnp.where(takes_in, other, own), ((1,), (1,)))
        for k in range(SIDE):
            block = block_of(swap_last((k - at_x[0]) & (SIDE - 1))).astype(F32)
            cols = slice(128 * k, 128 * (k + 1))
            copy_in[:, cols] = (block[0:W] - 0.02 * s_in[:, cols]).astype(BF16)
            copy_out[:, cols] = (block[W:] - 0.02 * s_out[:, cols]).astype(BF16)

    pairs = ((old_0a, old_0b), (old_1a, old_1b), (old_3a, old_3b), (old_2a, old_2b))
    for step, (near, far) in enumerate(pairs):

        @pl.when(n == step)
        def _():
            write(lambda r: jnp.where(r < 2, near[r & 1], far[r & 1]))


def final(core, at_x, at_z, full, mark, bases, weights, own, other, old):
    shape = jax.ShapeDtypeStruct

    def whole(s):
        return pl.BlockSpec(s, lambda *_: (0,) * len(s))

    def place(i, at_z):
        return (at_z[0] + swap_last(i)) & (SIDE - 1)

    tall = whole((W, 128))
    tile = pl.BlockSpec((512, RANK), lambda i, core, at_x, at_z: (place(i, at_z), 0))
    copy = pl.BlockSpec((W, 512), lambda i, core, at_x, at_z: (0, place(i, at_z)))
    return pl.pallas_call(
        final_kernel,
        grid_spec=pltpu.PrefetchScalarGridSpec(
            num_scalar_prefetch=3,
            grid=(SIDE,),
            in_specs=[
                whole((RANK, 2 * W)),
                whole((8, 128)),
                whole((2 * 128, RANK)),
                whole((2 * W, 128)),
                tile,
                tile,
                *[whole((2, 2 * W, 128))] * 8,
            ],
            out_specs=(tall, tall, copy, tall, tall, copy),
            scratch_shapes=[pltpu.VMEM((2 * W, RANK), BF16)],
        ),
        out_shape=(
            shape((W, 128), F32),
            shape((W, 128), F32),
            shape((W, 2048), BF16),
            shape((W, 128), F32),
            shape((W, 128), F32),
            shape((W, 2048), BF16),
        ),
        name="final",
        compiler_params=LIMIT,
        cost_estimate=pl.CostEstimate(
            flops=700_000_000, bytes_accessed=10_000_000, transcendentals=0
        ),
    )(core, at_x, at_z, full, mark, bases, weights, own, other, *old)


def shards(
    h_saved,
    conv_cotan,
    lru_out,
    out_cotan,
    basis_in,
    basis_out,
    weight_in,
    weight_out,
    first_in,
    second_in,
    first_out,
    second_out,
):
    core = lax.axis_index("tp_1").astype(jnp.int32).reshape(1)
    at_z = lax.axis_index("fs_0").astype(jnp.int32).reshape(1)
    at_x = lax.axis_index("fs_1").astype(jnp.int32).reshape(1)

    packed, bases = pack(core, at_x, at_z, weight_in.T, weight_out, basis_in, basis_out)

    basis_own = lax.all_to_all(bases, FS, 0, 0, tiled=True).reshape(-1, RANK)
    basis_other = swapped(basis_own)

    pieces = [packed]
    for d in (1, 3, 2):
        pieces.append(shifted(packed, "fs_1", -d))
    old_weights = lax.optimization_barrier(
        jnp.concatenate((weight_in.T, weight_out), axis=0)
    )
    pieces[0] = old_weights.astype(BF16)
    halves = [lax.optimization_barrier(jnp.stack(pieces[k : k + 2])) for k in (0, 2)]
    old = list(halves)
    for d in (1, 3):
        for k in range(2):
            old.append(shifted(halves[k], "fs_0", -d))
    old.append(shifted(old[2], "fs_0", -1))
    old.append(shifted(old[5], "fs_0", -3))

    conv, lru = conv_cotan.T, lru_out.T
    conv_came = swapped(conv)
    lru_came = swapped(lru)
    grads = grad(core, conv, conv_came, lru, lru_came, h_saved, out_cotan)
    part = project(grads, basis_own)
    arrived = lax.all_to_all(
        part.reshape(PEERS, ROWS, 2 * W), FS, split_axis=0, concat_axis=0, tiled=True
    )
    old_moments = lax.optimization_barrier(
        jnp.concatenate((first_in, second_in, first_out, second_out), axis=0)
    )
    own_bases = lax.optimization_barrier(jnp.concatenate((basis_in, basis_out), axis=0))
    proj_own, proj_given, squares = collect(arrived)
    totals = lax.all_to_all(squares, EVERY, 0, 0, tiled=True)
    proj_other = swapped(proj_given)
    first_a, second_a, first_b, second_b, dirs = apply(
        core, totals, proj_own, proj_other, old_moments
    )
    full = lax.all_to_all(dirs, FS, 0, 0, tiled=True).reshape(RANK, 2 * W)
    mark = lax.optimization_barrier(full[:8, :128])
    step_in, new_in, copy_in, step_out, new_out, copy_out = final(
        core, at_x, at_z, full, mark, own_bases, old_weights, basis_own, basis_other, old
    )
    return (
        step_in.T,
        new_in.T,
        copy_in.T,
        first_a,
        second_a,
        step_out,
        new_out,
        copy_out,
        first_b,
        second_b,
    )


def solution(mesh):
    finer = Mesh(mesh.devices.reshape(4, 4, 4, 2), EVERY)
    placed = (
        P(FS, None),
        P(FS, TP),
        P(FS, TP),
        P(FS, None),
        P(FS, None),
        P(FS, None),
        P(FS, TP),
        P(TP, FS),
        P(FS, TP),
        P(FS, TP),
        P(FS, TP),
        P(FS, TP),
    )
    return jax.shard_map(
        shards,
        mesh=finer,
        in_specs=placed,
        out_specs=(
            P(FS, TP),
            P(FS, TP),
            P(None, TP),
            P(FS, TP),
            P(FS, TP),
            P(TP, FS),
            P(TP, FS),
            P(TP, None),
            P(FS, TP),
            P(FS, TP),
        ),
        check_vma=False,
    )
```

```python
import math

import jax
import jax.numpy as jnp
from jax import lax
from jax.experimental import pallas as pl
from jax.experimental.pallas import tpu as pltpu
from jax.sharding import Mesh
from jax.sharding import PartitionSpec as P

D_RNN = 2560
RANK = 256
FS = ("fs_0", "fs_1")
TP = ("tp_0", "tp_1")
EVERY = ("fs_0", "fs_1", "tp_0", "tp_1")
BF16 = jnp.bfloat16
F32 = jnp.float32

W = 320
ROWS = 16
PEERS = 16
SIDE = 4

LIMIT = pltpu.CompilerParams(vmem_limit_bytes=20 << 20)
VMEM = pl.BlockSpec(memory_space=pltpu.VMEM)
SMEM = pl.BlockSpec(memory_space=pltpu.SMEM)


def swapped(array):
    return lax.ppermute(array, "tp_1", [(0, 1), (1, 0)])


def shifted(array, axis, by):
    return lax.ppermute(array, axis, [(i, (i + by) % SIDE) for i in range(SIDE)])


def contract(a, b, dims):
    return lax.dot_general(a, b, (dims, ((), ())), preferred_element_type=F32)


def pack_kernel(core, at_x, at_z, w_in, w_out, b_in, b_out, weights, bases):
    weights[0:W, :] = w_in[...].astype(BF16)
    weights[W : 2 * W, :] = w_out[...].astype(BF16)
    mine = jnp.where(core[0] == 0, b_in[...], b_out[...])
    for i in range(PEERS):
        bases[i] = mine


def pack(*args):
    return pl.pallas_call(
        pack_kernel,
        out_shape=(
            jax.ShapeDtypeStruct((2 * W, 128), BF16),
            jax.ShapeDtypeStruct((PEERS, 128, RANK), BF16),
        ),
        grid=(1,),
        in_specs=[
            SMEM,
            SMEM,
            SMEM,
            pl.BlockSpec((W, 128), lambda i: (0, 0)),
            pl.BlockSpec((W, 128), lambda i: (0, 0)),
            pl.BlockSpec((128, RANK), lambda i: (0, 0)),
            pl.BlockSpec((128, RANK), lambda i: (0, 0)),
        ],
        out_specs=(
            pl.BlockSpec((2 * W, 128), lambda i: (0, 0)),
            pl.BlockSpec((PEERS, 128, RANK), lambda i: (0, 0, 0)),
        ),
        name="pack",
        cost_estimate=pl.CostEstimate(flops=10**6, bytes_accessed=500_000, transcendentals=0),
    )(*args)


GRAD_TILE = 512
GRAD_TILES = 2048 // GRAD_TILE


def grad_kernel(core, conv, conv_came, lru, lru_came, h, o, out, wide, tall, sems):
    def tile(source, k):
        cols = slice(k * GRAD_TILE, (k + 1) * GRAD_TILE)
        return pltpu.make_async_copy(source.at[:, cols], tall.at[k], sems.at[k])

    def half(source, k):
        return pltpu.make_async_copy(
            source, wide.at[k * W : (k + 1) * W], sems.at[GRAD_TILES + k]
        )

    def start(own, came, source):
        half(own, 0).start()
        half(came, 1).start()
        for k in range(GRAD_TILES):
            tile(source, k).start()

    @pl.when(core[0] == 0)
    def _():
        start(conv, conv_came, h)

    @pl.when(core[0] != 0)
    def _():
        start(lru, lru_came, o)

    half(conv, 0).wait()
    half(conv_came, 1).wait()
    for k in range(GRAD_TILES):
        tile(h, k).wait()
        out[:, k * GRAD_TILE : (k + 1) * GRAD_TILE] = jnp.dot(
            wide[...], tall[k], preferred_element_type=F32
        ).astype(BF16)


def grad(*args):
    return pl.pallas_call(
        grad_kernel,
        in_specs=[SMEM] + [pl.BlockSpec(memory_space=pltpu.HBM)] * 6,
        out_specs=VMEM,
        out_shape=jax.ShapeDtypeStruct((2 * W, 2048), BF16),
        scratch_shapes=[
            pltpu.VMEM((2 * W, 2048), BF16),
            pltpu.VMEM((GRAD_TILES, 2048, GRAD_TILE), BF16),
            pltpu.SemaphoreType.DMA((GRAD_TILES + 2,)),
        ],
        name="grad",
        compiler_params=pltpu.CompilerParams(vmem_limit_bytes=63 << 20),
        cost_estimate=pl.CostEstimate(
            flops=4 * 2048 * 2048 * W, bytes_accessed=14_000_000, transcendentals=0
        ),
    )(*args)


PROJECT_TILES = 4


def project_kernel(grads, basis, out, grads_in, basis_in, sems):
    depth = 2048 // PROJECT_TILES
    copies = []
    for k in range(PROJECT_TILES):
        at = slice(k * depth, (k + 1) * depth)
        copies.append(
            (
                pltpu.make_async_copy(basis.at[at], basis_in.at[k], sems.at[0, k]),
                pltpu.make_async_copy(grads.at[:, at], grads_in.at[k], sems.at[1, k]),
            )
        )
    for group in copies:
        for copy in group:
            copy.start()
    mine = jnp.zeros((W, RANK), F32)
    other = jnp.zeros((W, RANK), F32)
    for k in range(PROJECT_TILES):
        for copy in copies[k]:
            copy.wait()
        mine = mine + jnp.dot(grads_in[k, 0:W], basis_in[k], preferred_element_type=F32)
        other = other + jnp.dot(grads_in[k, W:], basis_in[k], preferred_element_type=F32)
    out[:, 0:W] = mine.T.astype(BF16)
    out[:, W:] = other.T.astype(BF16)


def project(grads, basis):
    depth = 2048 // PROJECT_TILES
    return pl.pallas_call(
        project_kernel,
        in_specs=[pl.BlockSpec(memory_space=pltpu.HBM)] * 2,
        out_specs=VMEM,
        out_shape=jax.ShapeDtypeStruct((RANK, 2 * W), BF16),
        scratch_shapes=[
            pltpu.VMEM((PROJECT_TILES, 2 * W, depth), BF16),
            pltpu.VMEM((PROJECT_TILES, depth, RANK), BF16),
            pltpu.SemaphoreType.DMA((2, PROJECT_TILES)),
        ],
        name="project",
        compiler_params=pltpu.CompilerParams(vmem_limit_bytes=63 << 20),
        cost_estimate=pl.CostEstimate(
            flops=4 * 2048 * RANK * W, bytes_accessed=4_000_000, transcendentals=0
        ),
    )(grads, basis)


def collect_kernel(arrived, kept, given, squares):
    total = arrived[0].astype(F32)
    for i in range(1, PEERS):
        total = total + arrived[i].astype(F32)
    kept[...] = total[:, 0:W]
    given[...] = total[:, W:]
    sum_ = jnp.sum(jnp.sum(total * total, axis=0, keepdims=True), axis=1, keepdims=True)
    squares[...] = jnp.broadcast_to(sum_.reshape(1, 1, 1), (128, 1, 128))


def collect(arrived):
    return pl.pallas_call(
        collect_kernel,
        out_shape=(
            jax.ShapeDtypeStruct((ROWS, W), F32),
            jax.ShapeDtypeStruct((ROWS, W), F32),
            jax.ShapeDtypeStruct((128, 1, 128), F32),
        ),
        in_specs=[VMEM],
        out_specs=(VMEM,) * 3,
        name="collect",
        compiler_params=LIMIT,
        cost_estimate=pl.CostEstimate(flops=10**6, bytes_accessed=500_000, transcendentals=0),
    )(arrived)


def apply_kernel(
    core, totals, kept, came, old, nf_in, nv_in, nf_out, nv_out, dirs
):
    takes_in = core[0] == 0
    total = jnp.sum(totals[...], axis=0)[:, 0:1]
    factor = math.sqrt(2.0 * RANK * D_RNN) * lax.rsqrt(total + 1e-06)
    mine = kept[...]
    other = came[...]

    def moments(scaled, at, new_first, new_second):
        first = 0.8 * old[at : at + ROWS] + 0.2 * scaled
        second = 0.9 * old[at + ROWS : at + 2 * ROWS] + 0.1 * scaled * scaled
        new_first[...] = first
        new_second[...] = second
        return (first / (jnp.sqrt(second) + 1e-08)).astype(BF16)

    both = jnp.concatenate(
        (
            moments(factor * jnp.where(takes_in, mine, other), 0, nf_in, nv_in),
            moments(factor * jnp.where(takes_in, other, mine), 2 * ROWS, nf_out, nv_out),
        ),
        axis=1,
    )
    for i in range(PEERS):
        dirs[i] = both


def apply(*args):
    row = jax.ShapeDtypeStruct((ROWS, W), F32)
    return pl.pallas_call(
        apply_kernel,
        out_shape=(row, row, row, row, jax.ShapeDtypeStruct((PEERS, ROWS, 2 * W), BF16)),
        in_specs=[SMEM] + [VMEM] * 4,
        out_specs=(VMEM,) * 5,
        name="apply",
        compiler_params=LIMIT,
        cost_estimate=pl.CostEstimate(flops=10**6, bytes_accessed=500_000, transcendentals=0),
    )(*args)


def swap_last(n):
    return n ^ (n >> 1)


def final_kernel(
    at_x,
    at_z,
    full,
    mark,
    bases,
    weights,
    whole_in,
    whole_out,
    old_0a,
    old_0b,
    old_1a,
    old_1b,
    old_3a,
    old_3b,
    old_2a,
    old_2b,
    step_in,
    new_in,
    copy_in,
    step_out,
    new_out,
    copy_out,
    turned,
):
    n = pl.program_id(0)

    @pl.when(n == 0)
    def _():
        turned[...] = full[...].astype(F32).T.astype(BF16)
        own_in = contract(turned[0:W], bases[0:128], ((1,), (1,)))
        own_out = contract(turned[W:], bases[128:], ((1,), (1,)))
        step_in[...] = own_in
        step_out[...] = own_out
        new_in[...] = weights[0:W] - 0.02 * own_in
        new_out[...] = weights[W:] - 0.02 * own_out

    def write(block_of):
        s_in = contract(turned[0:W], whole_in[...], ((1,), (1,)))
        s_out = contract(turned[W:], whole_out[...], ((1,), (1,)))
        for k in range(SIDE):
            block = block_of(swap_last((k - at_x[0]) & (SIDE - 1))).astype(F32)
            cols = slice(128 * k, 128 * (k + 1))
            copy_in[:, cols] = (block[0:W] - 0.02 * s_in[:, cols]).astype(BF16)
            copy_out[:, cols] = (block[W:] - 0.02 * s_out[:, cols]).astype(BF16)

    pairs = ((old_0a, old_0b), (old_1a, old_1b), (old_3a, old_3b), (old_2a, old_2b))
    for step, (near, far) in enumerate(pairs):

        @pl.when(n == step)
        def _():
            write(lambda r: jnp.where(r < 2, near[r & 1], far[r & 1]))


def final(at_x, at_z, full, mark, bases, weights, whole_in, whole_out, old):
    shape = jax.ShapeDtypeStruct

    def whole(s):
        return pl.BlockSpec(s, lambda *_: (0,) * len(s))

    def place(i, at_z):
        return (at_z[0] + swap_last(i)) & (SIDE - 1)

    tall = whole((W, 128))
    tile = pl.BlockSpec((512, RANK), lambda i, at_x, at_z: (place(i, at_z), 0))
    copy = pl.BlockSpec((W, 512), lambda i, at_x, at_z: (0, place(i, at_z)))
    return pl.pallas_call(
        final_kernel,
        grid_spec=pltpu.PrefetchScalarGridSpec(
            num_scalar_prefetch=2,
            grid=(SIDE,),
            in_specs=[
                whole((RANK, 2 * W)),
                whole((8, 128)),
                whole((2 * 128, RANK)),
                whole((2 * W, 128)),
                tile,
                tile,
                *[whole((2, 2 * W, 128))] * 8,
            ],
            out_specs=(tall, tall, copy, tall, tall, copy),
            scratch_shapes=[pltpu.VMEM((2 * W, RANK), BF16)],
        ),
        out_shape=(
            shape((W, 128), F32),
            shape((W, 128), F32),
            shape((W, 2048), BF16),
            shape((W, 128), F32),
            shape((W, 128), F32),
            shape((W, 2048), BF16),
        ),
        name="final",
        compiler_params=LIMIT,
        cost_estimate=pl.CostEstimate(
            flops=700_000_000, bytes_accessed=10_000_000, transcendentals=0
        ),
    )(at_x, at_z, full, mark, bases, weights, whole_in, whole_out, *old)


def shards(
    h_saved,
    conv_cotan,
    lru_out,
    out_cotan,
    basis_in,
    basis_out,
    weight_in,
    weight_out,
    first_in,
    second_in,
    first_out,
    second_out,
):
    core = lax.axis_index("tp_1").astype(jnp.int32).reshape(1)
    at_z = lax.axis_index("fs_0").astype(jnp.int32).reshape(1)
    at_x = lax.axis_index("fs_1").astype(jnp.int32).reshape(1)

    packed, bases = pack(core, at_x, at_z, weight_in.T, weight_out, basis_in, basis_out)

    basis_own = lax.all_to_all(bases, FS, 0, 0, tiled=True).reshape(-1, RANK)
    basis_other = swapped(basis_own)

    pieces = [packed]
    for d in (1, 3, 2):
        pieces.append(shifted(packed, "fs_1", -d))
    old_weights = lax.optimization_barrier(
        jnp.concatenate((weight_in.T, weight_out), axis=0)
    )
    pieces[0] = old_weights.astype(BF16)
    halves = [lax.optimization_barrier(jnp.stack(pieces[k : k + 2])) for k in (0, 2)]
    old = list(halves)
    for d in (1, 3):
        for k in range(2):
            old.append(shifted(halves[k], "fs_0", -d))
    old.append(shifted(old[2], "fs_0", -1))
    old.append(shifted(old[5], "fs_0", -3))

    conv, lru = conv_cotan.T, lru_out.T
    conv_came = swapped(conv)
    lru_came = swapped(lru)
    grads = grad(core, conv, conv_came, lru, lru_came, h_saved, out_cotan)
    part = project(grads, basis_own)
    arrived = lax.all_to_all(
        part.reshape(PEERS, ROWS, 2 * W), FS, split_axis=0, concat_axis=0, tiled=True
    )
    old_moments = lax.optimization_barrier(
        jnp.concatenate((first_in, second_in, first_out, second_out), axis=0)
    )
    own_bases = lax.optimization_barrier(jnp.concatenate((basis_in, basis_out), axis=0))
    proj_own, proj_given, squares = collect(arrived)
    totals = lax.all_to_all(squares, EVERY, 0, 0, tiled=True)
    proj_other = swapped(proj_given)
    first_a, second_a, first_b, second_b, dirs = apply(
        core, totals, proj_own, proj_other, old_moments
    )
    full = lax.all_to_all(dirs, FS, 0, 0, tiled=True).reshape(RANK, 2 * W)
    mark = lax.optimization_barrier(full[:8, :128])
    sides = lax.optimization_barrier(
        (
            jnp.where(core[0] == 0, basis_own, basis_other),
            jnp.where(core[0] == 0, basis_other, basis_own),
        )
    )
    step_in, new_in, copy_in, step_out, new_out, copy_out = final(
        at_x, at_z, full, mark, own_bases, old_weights, *sides, old
    )
    return (
        step_in.T,
        new_in.T,
        copy_in.T,
        first_a,
        second_a,
        step_out,
        new_out,
        copy_out,
        first_b,
        second_b,
    )


def solution(mesh):
    finer = Mesh(mesh.devices.reshape(4, 4, 4, 2), EVERY)
    placed = (
        P(FS, None),
        P(FS, TP),
        P(FS, TP),
        P(FS, None),
        P(FS, None),
        P(FS, None),
        P(FS, TP),
        P(TP, FS),
        P(FS, TP),
        P(FS, TP),
        P(FS, TP),
        P(FS, TP),
    )
    return jax.shard_map(
        shards,
        mesh=finer,
        in_specs=placed,
        out_specs=(
            P(FS, TP),
            P(FS, TP),
            P(None, TP),
            P(FS, TP),
            P(FS, TP),
            P(TP, FS),
            P(TP, FS),
            P(TP, None),
            P(FS, TP),
            P(FS, TP),
        ),
        check_vma=False,
    )
```
